32 devices in a mesh: grp: 2 (over y), kv: 4 (over z), tp: 4 (over x, core).
Axes of the slice: x: 2, y: 2, z: 4, core: 2. Of those that a mesh axis runs over, the one named last changes fastest.
Arguments:
- piece_rows: bfloat16 [512, 2048], P(('grp', 'kv')), parts along dimension 0, may hold values from -6 to 6
- dec_rows: bfloat16 [16, 2048], P(('grp', 'kv')), parts along dimension 0, may hold values from -6 to 6
- norm_gain: float32 [2048], replicated, may hold values from 0.1 to 1.9
- w_query: bfloat16 [2048, 1024], P(None, 'tp'), may hold values from -0.25 to 0.25
- w_key: bfloat16 [2048, 256], P(None, 'tp'), may hold values from -0.125 to 0.125
- w_value: bfloat16 [2048, 256], P(None, 'tp'), may hold values from -0.125 to 0.125
- w_forget: bfloat16 [2048, 16], P(None, 'tp'), may hold values from -0.125 to 0.125
- forget_bias: float32 [16], P('tp'), may hold values from 3 to 12
- piece_decay: float32 [16, 512], P('tp', ('grp', 'kv')), parts along dimension 1, may hold values from -3 to 0
- cache_kv: bfloat16 [6144, 4, 128], P(('grp', 'kv'), 'tp'), parts along dimension 0, may hold values from -150 to 150
- cache_gate: float32 [16, 6144], P('tp', ('grp', 'kv')), parts along dimension 1, may hold values from -156.6 to 0, as said below
- dec_cache: bfloat16 [16, 3072, 4, 128], P(('grp', 'kv'), None, 'tp'), parts along dimension 0, may hold values from -150 to 150
- dec_gate: float32 [16, 16, 3072], P(('grp', 'kv'), 'tp'), parts along dimension 0, may hold values from -156.6 to 0, as said below
- dec_lengths: int32 [16], P(('grp', 'kv')), parts along dimension 0, may hold values from 1 to 3072, as said below
- w_out: bfloat16 [1024, 2048], P(None, 'tp'), may hold values from -0.75 to 0.75
Outputs:
- piece_out: bfloat16 [512, 2048], P(('grp', 'kv'), 'tp'), parts along dimension 0
- dec_out: bfloat16 [16, 2048], P(('grp', 'kv'), 'tp'), parts along dimension 0
The draws below stay inside these ranges and needn't reach their ends.
There are 2 independent parts, one for each index of `grp`. The reference program is written for one: setup_inputs(seed, part) draws one part's arguments, and reference() takes and returns one part's arrays. A program takes and returns all parts, laid end to end along the dimension named above; an argument that names none is the same for every part. Nothing has to cross between parts.
Inputs may be any that keep to these rules, and one draw needn't show every extreme that they name: `cache_gate`: each head's values never fall from one position to the next and are 0 at the last cached position. `dec_gate`: each sequence's and head's values never rise from one position to the next. Sequence b's cache holds its first dec_lengths[b] positions; in each part some sequence holds 3072.
All inputs are finite; a program needn't handle non-finite values.
Results may differ from the reference program's by a relative error of at most 0.006.
The reference program's roundings to bfloat16 on the way count: a program that leaves them out, or rounds other values in their place, can miss the bound.
Values may be sent and summed in bfloat16 or wider, within the bound.
A program may use at most 64 MiB of HBM per device.

```python
import math
import jax
import jax.numpy as jnp
from jax import lax

D = 2048
HEADS = 16
KV_HEADS = 4
HEAD_DIM = 64
PIECE_DEV = 64
PAST_DEV = 768
DEC_LEN = 3072
PIECE = 256
PAST = 3072
DEC_SEQS = 8
N_KV = 4


def slow_heads(key, shape):
    pick = jax.random.randint(key, shape, 0, 10)
    return pick < 5


def gate_logs(key, rows, span, blocks):
    gradual_heads = slow_heads(jax.random.fold_in(key, 1), (rows, 1))
    factor = jnp.exp(jax.random.uniform(jax.random.fold_in(key, 2), (rows, blocks), jnp.float32, math.log(0.4), math.log(2.5)))
    factor = jnp.repeat(factor, span // blocks, axis=1)
    gradual_decay_rate = jax.random.uniform(jax.random.fold_in(key, 3), (rows, span), jnp.float32, 0.2, 1.0) * factor / span
    quick_decay_rate = jax.random.uniform(jax.random.fold_in(key, 4), (rows, span), jnp.float32, 0.01, 0.05)
    chosen_locations = jax.random.randint(jax.random.fold_in(key, 5), (rows, 3), 0, span)
    layer_depth = jax.random.uniform(jax.random.fold_in(key, 6), (rows, 3), jnp.float32, 0.22, 0.7)
    target_location = jnp.arange(span, dtype=jnp.int32)
    sudden_spike = jnp.sum(jnp.where(target_location[None, None, :] == chosen_locations[:, :, None], layer_depth[:, :, None], 0.0), axis=1)
    return -jnp.where(gradual_heads, gradual_decay_rate + sudden_spike, quick_decay_rate)


def spiky(key, shape):
    base = jnp.clip(jax.random.normal(jax.random.fold_in(key, 1), shape, jnp.float32), -6.0, 6.0)
    return base.astype(jnp.bfloat16)


def draw_forget_bias(key, part):
    gradual_heads = slow_heads(jax.random.fold_in(key, 11), (HEADS,))
    slow_value = jax.random.uniform(jax.random.fold_in(key, 12), (HEADS,), jnp.float32, 10.0, 12.0)
    fast_value = jax.random.uniform(jax.random.fold_in(key, 13), (HEADS,), jnp.float32, 3.0, 4.5)
    return jnp.where(gradual_heads, slow_value, fast_value)


def draw_piece_decay(key, part):
    decay_rates = jnp.exp(jax.random.uniform(jax.random.fold_in(key, 21), (N_KV,), jnp.float32, math.log(0.0002), math.log(0.003)))
    decay_rates = jnp.repeat(decay_rates, PIECE_DEV)
    random_noise = jax.random.uniform(jax.random.fold_in(key, 22), (HEADS, PIECE), jnp.float32, 0.5, 1.5)
    chosen_locations = jax.random.randint(jax.random.fold_in(key, 23), (3,), 0, PIECE)
    layer_depth = jax.random.uniform(jax.random.fold_in(key, 24), (HEADS, 3), jnp.float32, 0.22, 0.7)
    target_location = jnp.arange(PIECE, dtype=jnp.int32)
    sudden_spike = jnp.sum(jnp.where(target_location[None, None, :] == chosen_locations[None, :, None], layer_depth[:, :, None], 0.0), axis=1)
    return -(decay_rates[None, :] * random_noise + sudden_spike)


def draw_cache_gate(key, part):
    logs = gate_logs(jax.random.fold_in(key, 31), HEADS, PAST, N_KV)
    return jnp.flip(jnp.cumsum(jnp.flip(logs, 1), axis=1), 1) - logs


def draw_dec_gate(key, part):
    logs = gate_logs(jax.random.fold_in(key, 41), DEC_SEQS * HEADS, DEC_LEN, 1)
    return jnp.cumsum(logs, axis=1).reshape(DEC_SEQS, HEADS, DEC_LEN)


def draw_cache_kv(key, part):
    return spiky(jax.random.fold_in(key, 51), (PAST, KV_HEADS, 2 * HEAD_DIM))


def draw_dec_cache(key, part):
    return spiky(jax.random.fold_in(key, 61), (DEC_SEQS, DEC_LEN, KV_HEADS, 2 * HEAD_DIM))


def draw_dec_lengths(key, part):
    base = jax.random.randint(jax.random.fold_in(key, 71), (DEC_SEQS,), 1, DEC_LEN + 1)
    fullest = jax.random.randint(jax.random.fold_in(key, 72), (), 0, DEC_SEQS)
    slot_index = jnp.arange(DEC_SEQS, dtype=jnp.int32)
    return jnp.where(slot_index == fullest, DEC_LEN, base).astype(jnp.int32)


def level_of(key, shape, pieces, low, high):
    level = 1.0
    for dim, blocks in pieces:
        steps = jax.random.uniform(jax.random.fold_in(jax.random.fold_in(key, 6), dim), (blocks,), jnp.float32, low / len(pieces), high / len(pieces))
        level = level * jnp.repeat(jnp.exp(steps), shape[dim] // blocks).reshape((-1,) + (1,) * (len(shape) - 1 - dim))
    return level


def scatter_about(stream_key, dims, spread, most, pieces=(), held_as=jnp.bfloat16):
    result = spread * jax.random.normal(stream_key, dims, jnp.float32)
    if pieces:
        result = result * level_of(stream_key, dims, pieces, -0.22, 0.18)
    return jnp.clip(result, -most, most).astype(held_as)


def setup_inputs(seed: int = 0, part: int = 0) -> dict:
    key_of = jax.random.split(jax.random.key(seed), 16)
    own_keys = jax.random.split(jax.random.fold_in(key_of[15], part), 16)
    piece_rows = scatter_about(own_keys[0], (PIECE, D), 1.0, 6.0, ((0, 4),))
    dec_rows = scatter_about(own_keys[1], (DEC_SEQS, D), 1.0, 6.0, ((0, 4),))
    norm_gain = jnp.clip(1.0 + 0.18 * jax.random.normal(key_of[2], (D,), jnp.float32), 0.1, 1.9)
    w_query = scatter_about(key_of[3], (D, HEADS * HEAD_DIM), (D // 4) ** -0.5, 0.25, ((1, 4),))
    w_key = scatter_about(key_of[4], (D, KV_HEADS * HEAD_DIM), D ** -0.5, 0.125, ((1, 4),))
    w_value = scatter_about(key_of[5], (D, KV_HEADS * HEAD_DIM), D ** -0.5, 0.125, ((1, 4),))
    w_forget = scatter_about(key_of[6], (D, HEADS), D ** -0.5, 0.125, ((1, 4),))
    forget_bias = draw_forget_bias(jax.random.fold_in(key_of[15], 71), part)
    piece_decay = draw_piece_decay(jax.random.fold_in(jax.random.fold_in(key_of[15], part), 71), part)
    cache_kv = draw_cache_kv(jax.random.fold_in(jax.random.fold_in(key_of[15], part), 71), part)
    cache_gate = draw_cache_gate(jax.random.fold_in(jax.random.fold_in(key_of[15], part), 71), part)
    dec_cache = draw_dec_cache(jax.random.fold_in(jax.random.fold_in(key_of[15], part), 71), part)
    dec_gate = draw_dec_gate(jax.random.fold_in(jax.random.fold_in(key_of[15], part), 71), part)
    dec_lengths = draw_dec_lengths(jax.random.fold_in(jax.random.fold_in(key_of[15], part), 71), part)
    w_out = scatter_about(key_of[14], (HEADS * HEAD_DIM, D), HEAD_DIM ** -0.5, 0.75, ((1, 4),))
    return dict(piece_rows=piece_rows, dec_rows=dec_rows, norm_gain=norm_gain, w_query=w_query, w_key=w_key, w_value=w_value, w_forget=w_forget, forget_bias=forget_bias, piece_decay=piece_decay, cache_kv=cache_kv, cache_gate=cache_gate, dec_cache=dec_cache, dec_gate=dec_gate, dec_lengths=dec_lengths, w_out=w_out)


def norm_rows(rows, gain):
    wide = rows.astype(jnp.float32)
    scale = lax.rsqrt(lax.optimization_barrier(jnp.mean(wide * wide, axis=-1, keepdims=True)) + 1e-06)
    return (wide * scale * gain.astype(jnp.float32)).astype(jnp.bfloat16)

def merge_state(state, part):
    peak, total, numer = state
    new_peak, new_total, new_numer = part
    highest = jnp.maximum(peak, new_peak)
    keep = jnp.exp(peak - highest)
    fresh = jnp.exp(new_peak - highest)
    return (highest, total * keep + new_total * fresh, numer * keep[..., None] + new_numer * fresh[..., None])

def group_partial(query, query_index, group_kv, group_bias, group, past_rows, new_rows):
    head_width = query.shape[-1]
    keys = group_kv[..., :head_width].astype(jnp.float32)
    values = group_kv[..., head_width:].astype(jnp.float32)
    score = jnp.einsum('bkgd,nkd->bkgn', query.astype(jnp.float32), keys)
    score = score * head_width ** (-0.5) + group_bias[None]
    rank = jnp.arange(group_kv.shape[0], dtype=jnp.int32)
    new_index = group * new_rows + rank - past_rows
    visible = (rank < past_rows)[None, :] | (new_index[None, :] <= query_index[:, None])
    score = jnp.where(visible[:, None, None, :], score, -jnp.inf)
    peak = lax.optimization_barrier(jnp.max(score, axis=-1))
    weight = jnp.exp(score - peak[..., None])
    total = lax.optimization_barrier(jnp.sum(weight, axis=-1))
    rounded = lax.optimization_barrier(weight.astype(jnp.bfloat16))
    numer = jnp.einsum('bkgn,nkd->bkgd', rounded.astype(jnp.float32), values)
    return (peak, total, numer)

def decode_attention(query, new_key, new_value, new_gate, cache, gate, lengths):
    seqs, pairs_here, group_size, head_width = query.shape
    span = cache.shape[1]
    keys = cache[..., :head_width].astype(jnp.float32)
    values = cache[..., head_width:].astype(jnp.float32)
    target_location = jnp.arange(span, dtype=jnp.int32)
    last_gate = lax.optimization_barrier(jnp.sum(jnp.where(target_location[None, None, :] == lengths[:, None, None] - 1, gate, 0.0), axis=-1))
    score = jnp.einsum('skgd,slkd->skgl', query.astype(jnp.float32), keys) * head_width ** (-0.5)
    score = score - gate.reshape(seqs, pairs_here, group_size, span)
    score = jnp.where((target_location[None, :] < lengths[:, None])[:, None, None, :], score, -jnp.inf)
    own = jnp.einsum('skgd,skd->skg', query.astype(jnp.float32), new_key.astype(jnp.float32)) * head_width ** (-0.5)
    own = own - (last_gate + new_gate).reshape(seqs, pairs_here, group_size)
    peak = jnp.maximum(lax.optimization_barrier(jnp.max(score, axis=-1)), own)
    weight = jnp.exp(score - peak[..., None])
    own_weight = jnp.exp(own - peak)
    total = lax.optimization_barrier(jnp.sum(weight, axis=-1)) + own_weight
    rounded = lax.optimization_barrier(weight.astype(jnp.bfloat16))
    own_rounded = lax.optimization_barrier(own_weight.astype(jnp.bfloat16))
    numer = jnp.einsum('skgl,slkd->skgd', rounded.astype(jnp.float32), values)
    numer = numer + own_rounded.astype(jnp.float32)[..., None] * new_value[:, :, None, :].astype(jnp.float32)
    return numer / total[..., None]

def reference(piece_rows, dec_rows, norm_gain, w_query, w_key, w_value, w_forget, forget_bias, piece_decay, cache_kv, cache_gate, dec_cache, dec_gate, dec_lengths, w_out):
    group_size = HEADS // KV_HEADS
    normed = norm_rows(jnp.concatenate([piece_rows, dec_rows], axis=0), norm_gain)
    query = jnp.dot(normed, w_query, preferred_element_type=jnp.float32).astype(jnp.bfloat16)
    new_key = jnp.dot(normed, w_key, preferred_element_type=jnp.float32).astype(jnp.bfloat16)
    new_value = jnp.dot(normed, w_value, preferred_element_type=jnp.float32).astype(jnp.bfloat16)
    log_gate = jax.nn.log_sigmoid(jnp.dot(normed, w_forget, preferred_element_type=jnp.float32) + forget_bias)
    piece_gate = log_gate[:PIECE] + piece_decay.T
    new_bias = -jnp.cumsum(piece_gate, axis=0).T
    piece_kv = jnp.concatenate([new_key[:PIECE].reshape(PIECE, KV_HEADS, HEAD_DIM), new_value[:PIECE].reshape(PIECE, KV_HEADS, HEAD_DIM)], axis=-1)
    past_groups = cache_kv.reshape(N_KV, PAST_DEV, KV_HEADS, 2 * HEAD_DIM)
    new_groups = piece_kv.reshape(N_KV, PIECE_DEV, KV_HEADS, 2 * HEAD_DIM)
    past_bias = jnp.transpose(cache_gate.reshape(HEADS, N_KV, PAST_DEV), (1, 0, 2))
    fresh_bias = jnp.transpose(new_bias.reshape(HEADS, N_KV, PIECE_DEV), (1, 0, 2))
    all_query = query[:PIECE].reshape(PIECE, KV_HEADS, group_size, HEAD_DIM)
    query_index = jnp.arange(PIECE, dtype=jnp.int32)

    def visit(state, item):
        past, fresh, past_gate, fresh_gate, group = item
        block = jnp.concatenate([past, fresh], axis=0)
        bias = jnp.concatenate([past_gate, fresh_gate], axis=1).reshape(KV_HEADS, group_size, PAST_DEV + PIECE_DEV)
        part = group_partial(all_query, query_index, block, bias, group, PAST_DEV, PIECE_DEV)
        return (merge_state(state, part), None)
    start_state = (jnp.full((PIECE, KV_HEADS, group_size), -jnp.inf, jnp.float32), jnp.zeros((PIECE, KV_HEADS, group_size), jnp.float32), jnp.zeros((PIECE, KV_HEADS, group_size, HEAD_DIM), jnp.float32))
    state, _ = lax.scan(visit, start_state, (past_groups, new_groups, past_bias, fresh_bias, jnp.arange(N_KV, dtype=jnp.int32)))
    piece_attn = (state[2] / state[1][..., None]).reshape(PIECE, HEADS * HEAD_DIM).astype(jnp.bfloat16)
    dec_count = dec_rows.shape[0]
    dec_attn = decode_attention(query[PIECE:].reshape(dec_count, KV_HEADS, group_size, HEAD_DIM), new_key[PIECE:].reshape(dec_count, KV_HEADS, HEAD_DIM), new_value[PIECE:].reshape(dec_count, KV_HEADS, HEAD_DIM), log_gate[PIECE:], dec_cache, dec_gate, dec_lengths)
    dec_attn = dec_attn.reshape(dec_count, HEADS * HEAD_DIM).astype(jnp.bfloat16)
    piece_out = jnp.dot(piece_attn, w_out, preferred_element_type=jnp.float32).astype(jnp.bfloat16)
    dec_out = jnp.dot(dec_attn, w_out, preferred_element_type=jnp.float32).astype(jnp.bfloat16)
    return (piece_out, dec_out)
```

```python
import functools
import math

import jax
import jax.numpy as jnp
from jax import lax
from jax.experimental import pallas as pl
from jax.experimental.pallas import tpu as pltpu
from jax.sharding import PartitionSpec as P

MESH = pl.DeviceIdType.MESH
LOG2E = math.log2(math.e)
F32 = jnp.float32
BF16 = jnp.bfloat16
HIGH = lax.Precision.HIGHEST


def dot_nt(a, b, precision=None):
    return lax.dot_general(
        a, b, (((1,), (1,)), ((), ())), preferred_element_type=F32, precision=precision
    )


def dot_nn(a, b, precision=None):
    return lax.dot_general(
        a, b, (((1,), (0,)), ((), ())), preferred_element_type=F32, precision=precision
    )


def dot_tn(a, b, precision=None):
    return lax.dot_general(
        a, b, (((0,), (0,)), ((), ())), preferred_element_type=F32, precision=precision
    )


def iota(shape, dim):
    return lax.broadcasted_iota(jnp.int32, shape, dim)


def loop(count, body, carry):
    if count <= 4:
        for k in range(count):
            carry = body(k, carry)
        return carry
    return lax.fori_loop(0, count, body, carry)


def normed_rows(rows, gain):
    wide = rows.astype(F32)
    scale = lax.rsqrt(jnp.mean(wide * wide, axis=-1, keepdims=True) + 1e-06)
    return wide * scale * gain


def kernel(
    n,
    t,
    piece_rows,
    dec_rows,
    gain_in,
    wq_in,
    wk_in,
    wv_in,
    wf_in,
    fb_in,
    decay_in,
    cache_in,
    cgate_in,
    dcache_in,
    dgate_in,
    lens_in,
    wo_in,
    piece_out,
    dec_out,
    rows,
    drows,
    gain,
    wq,
    wkv,
    wf,
    fb,
    decay,
    kv,
    vk,
    cgate,
    dcache,
    dgate,
    lens,
    wo,
    normed,
    qd,
    da,
    qbuf,
    tot,
    part,
    back,
    lse_part,
    lse_back,
    axp,
    axd,
    pbias,
    local_sem,
    q_send,
    q_recv,
    t_send,
    t_recv,
    p_send,
    p_recv,
    l_send,
    l_recv,
    a_send,
    a_recv,
    d_send,
    d_recv,
):
    me = lax.axis_index("kv")
    me_t = lax.axis_index("tp")
    count = piece_rows.shape[0]
    seqs = dec_rows.shape[0]
    past = cache_in.shape[0]
    wide = cache_in.shape[1]
    half = wide // 2
    heads = wf_in.shape[0]
    scale = half ** (-0.5) * LOG2E
    columns = heads * half

    def peer_at(k):
        down = n - 1 - k
        down = jnp.where(down <= me, down - 1, down)
        up = jnp.where(k >= me, k + 1, k)
        return jnp.where(me < n // 2, down, up)

    barrier = pltpu.get_barrier_semaphore()

    def greet(d, _):
        pl.semaphore_signal(
            barrier, inc=1, device_id={"kv": lax.rem(me + d + 1, n)}, device_id_type=MESH
        )
        return 0

    def greet_t(d, _):
        pl.semaphore_signal(
            barrier, inc=1, device_id={"tp": lax.rem(me_t + d + 1, t)}, device_id_type=MESH
        )
        return 0

    loop(n - 1, greet, 0)
    loop(t - 1, greet_t, 0)

    copies = {}
    for k, (name, src, dst) in enumerate(
        (
            ("rows", piece_rows, rows),
            ("drows", dec_rows, drows),
            ("gain", gain_in, gain),
            ("wq", wq_in, wq),
            ("wk", wk_in, wkv.at[pl.ds(0, half)]),
            ("wv", wv_in, wkv.at[pl.ds(half, half)]),
            ("wf", wf_in, wf),
            ("fb", fb_in, fb),
            ("decay", decay_in, decay),
            ("lens", lens_in, lens),
            ("dcache", dcache_in, dcache),
            ("dgate", dgate_in, dgate),
            ("cache", cache_in, kv.at[pl.ds(0, past)]),
            ("cgate", cgate_in, cgate),
            ("wo", wo_in, wo),
        )
    ):
        copy = pltpu.make_async_copy(src, dst, local_sem.at[k])
        copy.start()
        copies[name] = copy

    copies["rows"].wait()
    copies["drows"].wait()
    copies["gain"].wait()
    normed[0:count] = normed_rows(rows[...], gain[...]).astype(BF16)
    dec_normed = normed_rows(drows[...], gain[...])
    spare = normed.shape[0] - count
    normed[count:] = jnp.concatenate(
        [dec_normed, jnp.zeros((spare - seqs, dec_normed.shape[1]), F32)], axis=0
    ).astype(BF16)
    every = normed[...]
    copies["wf"].wait()
    copies["fb"].wait()
    copies["decay"].wait()
    raw = dot_nt(wf[...], every)
    row_of = iota((heads, 1), 0)
    bias = jnp.zeros((heads, 1), F32)
    for h in range(heads):
        bias = jnp.where(row_of == h, fb[h], bias)
    raw = raw + bias
    log_gate = jnp.minimum(raw, 0.0) - jnp.log1p(jnp.exp(-jnp.abs(raw)))
    piece_gate = log_gate[:, 0:count] + decay[...]
    upper = (iota((count, count), 0) <= iota((count, count), 1)).astype(F32)
    running = dot_nn(piece_gate, upper, HIGH)
    tot[0] = jnp.broadcast_to(running[:, count - 1 : count], tot.shape[1:])
    copies["wq"].wait()
    query = dot_nn(every, wq[...]).astype(BF16)
    qbuf[0] = query[0:count]

    pl.semaphore_wait(barrier, n - 1 + t - 1)

    def total_copy(peer):
        slot = lax.rem(peer - me + n, n)
        return pltpu.make_async_remote_copy(
            src_ref=tot.at[0],
            dst_ref=tot.at[slot],
            send_sem=t_send.at[slot],
            recv_sem=t_recv.at[slot],
            device_id={"kv": peer},
            device_id_type=MESH,
        )

    def query_copy(peer):
        slot = lax.rem(peer - me + n, n)
        return pltpu.make_async_remote_copy(
            src_ref=qbuf.at[0],
            dst_ref=qbuf.at[slot],
            send_sem=q_send.at[slot],
            recv_sem=q_recv.at[slot],
            device_id={"kv": peer},
            device_id_type=MESH,
        )

    def send_query(k, _):
        peer = peer_at(k)
        total_copy(peer).start()
        query_copy(peer).start()
        return 0

    loop(n - 1, send_query, 0)

    copies["wk"].wait()
    copies["wv"].wait()
    new_kv = dot_nt(every, wkv[...]).astype(BF16)
    copies["cache"].wait()
    kv[past : past + count] = new_kv[0:count]
    vk[...] = pltpu.roll(kv[...].astype(F32), half, 1).astype(BF16)
    copies["cgate"].wait()
    cgate[...] = cgate[...] * LOG2E

    lanes = seqs * heads
    qd[...] = jnp.zeros(qd.shape, F32)
    dec_query = query[count:].astype(F32)
    for b in range(seqs):
        for h in range(heads):
            qd[b * heads + h : b * heads + h + 1, 0:half] = dec_query[
                b : b + 1, h * half : (h + 1) * half
            ]
    q_dec = qd[...]
    dec_kv = new_kv[count:].astype(F32)
    copies["lens"].wait()
    copies["dgate"].wait()
    copies["dcache"].wait()
    span = dcache.shape[1]
    row = iota((lanes, 1), 0)
    length = jnp.zeros((lanes, 1), jnp.int32)
    own_kv = jnp.zeros((lanes, wide), F32)
    score = jnp.zeros((lanes, span), F32)
    for b in range(seqs):
        mine = (row >= b * heads) & (row < (b + 1) * heads)
        length = jnp.where(mine, lens[b], length)
        own_kv = jnp.where(mine, dec_kv[b : b + 1], own_kv)
        score = jnp.where(mine, dot_nt(q_dec.astype(BF16), dcache[b]), score)
    gate = jnp.concatenate([dgate[b] for b in range(seqs)], axis=0)
    new_gate = jnp.concatenate(
        [log_gate[:, count + b : count + b + 1] for b in range(seqs)], axis=0
    )
    place = iota((lanes, span), 1)
    last = jnp.sum(jnp.where(place == length - 1, gate, 0.0), axis=-1, keepdims=True)
    score = jnp.where(place < length, score * scale - gate * LOG2E, -jnp.inf)
    own = jnp.sum(q_dec * own_kv, axis=-1, keepdims=True) * scale - (last + new_gate) * LOG2E
    peak = jnp.maximum(jnp.max(score, axis=-1, keepdims=True), own)
    weight = jnp.exp2(score - peak)
    own_weight = jnp.exp2(own - peak)
    total = jnp.sum(weight, axis=-1, keepdims=True) + own_weight
    rounded = weight.astype(BF16)
    numer = own_weight.astype(BF16).astype(F32) * own_kv
    for b in range(seqs):
        mine = (row >= b * heads) & (row < (b + 1) * heads)
        numer = numer + jnp.where(mine, dot_nn(rounded, dcache[b]), 0.0)
    numer = numer / total
    da[...] = jnp.zeros(da.shape, F32)
    for b in range(seqs):
        for h in range(heads):
            at = b * heads + h
            da[b : b + 1, h * half : (h + 1) * half] = numer[at : at + 1, half:]
    axd[0] = da[...].astype(BF16)

    def head_copy(d, buf, send, recv):
        return pltpu.make_async_remote_copy(
            src_ref=buf.at[0],
            dst_ref=buf.at[d],
            send_sem=send.at[d],
            recv_sem=recv.at[d],
            device_id={"tp": lax.rem(me_t + d, t)},
            device_id_type=MESH,
        )

    for d in range(1, t):
        head_copy(d, axd, d_send, d_recv).start()

    def add_before(k, before):
        d = k + 1
        total_copy(lax.rem(me + d, n)).wait_recv()
        return before + jnp.where(d <= me, tot[d], 0.0)

    before = loop(n - 1, add_before, jnp.zeros(tot.shape[1:], F32))
    pbias[...] = -(running + before[:, 0:count]) * LOG2E

    low_lane = iota((count, wide), 1) < half
    low = jnp.where(low_lane, 1.0, 0.0).astype(BF16)
    high = jnp.where(low_lane, 0.0, 1.0).astype(BF16)
    lane = iota((count, wide), 1)

    def attend(q, seen):
        pairs = [q[:, p * wide : (p + 1) * wide] for p in range(heads // 2)]
        found = []
        stats = jnp.zeros((count, wide), F32)
        for odd, (mask, keys, values) in enumerate(((low, kv, vk), (high, vk, kv))):
            stacked = jnp.concatenate([p * mask for p in pairs], axis=0)
            old = dot_nt(stacked, keys[0:past])
            new = dot_nt(stacked, keys[past : past + count])
            old_weights, new_weights, sums = [], [], []
            for p in range(heads // 2):
                h = 2 * p + odd
                block = slice(p * count, (p + 1) * count)
                s_old = old[block] * scale + cgate[h : h + 1, :]
                s_new = jnp.where(seen, new[block] * scale + pbias[h : h + 1, :], -jnp.inf)
                top = jnp.maximum(
                    jnp.max(s_old, axis=-1, keepdims=True), jnp.max(s_new, axis=-1, keepdims=True)
                )
                w_old = jnp.exp2(s_old - top)
                w_new = jnp.exp2(s_new - top)
                amount = jnp.sum(w_old, axis=-1, keepdims=True) + jnp.sum(
                    w_new, axis=-1, keepdims=True
                )
                stats = jnp.where(lane == h, top + jnp.log2(amount), stats)
                old_weights.append(w_old.astype(BF16))
                new_weights.append(w_new.astype(BF16))
                sums.append(amount)
            out = dot_nn(jnp.concatenate(old_weights, axis=0), values[0:past])
            out = out + dot_nn(
                jnp.concatenate(new_weights, axis=0), values[past : past + count]
            )
            found.append(
                [out[p * count : (p + 1) * count] / sums[p] for p in range(heads // 2)]
            )
        merged = jnp.concatenate(
            [jnp.where(low_lane, found[0][p], found[1][p]) for p in range(heads // 2)], axis=1
        )
        return merged, jnp.transpose(stats)[0:heads, :]

    def part_copy(peer):
        slot = lax.rem(peer - me + n, n)
        return pltpu.make_async_remote_copy(
            src_ref=part.at[slot],
            dst_ref=back.at[slot],
            send_sem=p_send.at[slot],
            recv_sem=p_recv.at[slot],
            device_id={"kv": peer},
            device_id_type=MESH,
        )

    def lse_copy(peer):
        slot = lax.rem(peer - me + n, n)
        return pltpu.make_async_remote_copy(
            src_ref=lse_part.at[slot],
            dst_ref=lse_back.at[slot],
            send_sem=l_send.at[slot],
            recv_sem=l_recv.at[slot],
            device_id={"kv": peer},
            device_id_type=MESH,
        )

    def serve(k, _):
        peer = peer_at(n - 2 - k)
        came = lax.rem(me - peer + n, n)
        slot = lax.rem(peer - me + n, n)
        query_copy(lax.rem(me + came, n)).wait_recv()
        visible = iota((count, count), 0) * 0 + peer > me
        merged, lse = attend(qbuf[came], visible)
        part[slot] = merged.astype(BF16)
        lse_part[slot] = lse
        part_copy(peer).start()
        lse_copy(peer).start()
        return 0

    loop(n - 1, serve, 0)

    own_part, own_lse = attend(
        qbuf[0], iota((count, count), 1) <= iota((count, count), 0)
    )

    copies["wo"].wait()
    dec_mixed = jnp.zeros((axd.shape[1], wo.shape[1]), F32)
    for d in range(t):
        if d:
            head_copy(d, axd, d_send, d_recv).wait_recv()
        src = lax.rem(me_t - d + t, t)
        depth = pl.ds(pl.multiple_of(src * columns, columns), columns)
        dec_mixed = dec_mixed + dot_nn(axd[d], wo[depth, :])
    dec_out[...] = dec_mixed[0:seqs].astype(BF16)

    def top_of(k, top):
        d = k + 1
        lse_copy(lax.rem(me + d, n)).wait_recv()
        return jnp.maximum(top, lse_back[d])

    top = loop(n - 1, top_of, own_lse)
    own_share = jnp.exp2(own_lse - top)

    def sum_of(k, amount):
        return amount + jnp.exp2(lse_back[k + 1] - top)

    amount = loop(n - 1, sum_of, own_share)
    spread = (
        iota((heads, columns), 1) // half == iota((heads, columns), 0)
    ).astype(F32)

    def add_part(k, acc):
        d = k + 1
        share = dot_tn(jnp.exp2(lse_back[d] - top) / amount, spread, HIGH)
        part_copy(lax.rem(me + d, n)).wait_recv()
        return acc + back[d].astype(F32) * share

    attn = loop(n - 1, add_part, own_part * dot_tn(own_share / amount, spread, HIGH))
    axp[0] = attn.astype(BF16)
    for d in range(1, t):
        head_copy(d, axp, a_send, a_recv).start()
    mixed = jnp.zeros((count, wo.shape[1]), F32)
    for d in range(t):
        if d:
            head_copy(d, axp, a_send, a_recv).wait_recv()
        src = lax.rem(me_t - d + t, t)
        depth = pl.ds(pl.multiple_of(src * columns, columns), columns)
        mixed = mixed + dot_nn(axp[d], wo[depth, :])
    piece_out[...] = mixed.astype(BF16)

    def finish(k, _):
        peer = lax.rem(me + k + 1, n)
        total_copy(peer).wait_send()
        query_copy(peer).wait_send()
        part_copy(peer).wait_send()
        lse_copy(peer).wait_send()
        return 0

    loop(n - 1, finish, 0)
    for d in range(1, t):
        head_copy(d, axd, d_send, d_recv).wait_send()
        head_copy(d, axp, a_send, a_recv).wait_send()


def local(
    n,
    t,
    piece_rows,
    dec_rows,
    norm_gain,
    w_query,
    w_key,
    w_value,
    w_forget,
    forget_bias,
    piece_decay,
    cache_kv,
    cache_gate,
    dec_cache,
    dec_gate,
    dec_lengths,
    w_out,
):
    count, width = piece_rows.shape
    seqs = dec_rows.shape[0]
    past, _, wide = cache_kv.shape
    half = wide // 2
    heads = w_forget.shape[1]
    columns = heads * half
    span = dec_cache.shape[1]
    outs = w_out.shape[1]
    spare = 16
    dma = pltpu.SemaphoreType.DMA
    args = (
        piece_rows,
        dec_rows,
        norm_gain.reshape(1, width),
        w_query,
        w_key.T,
        w_value.T,
        w_forget.T,
        forget_bias,
        piece_decay,
        cache_kv.reshape(past, wide),
        cache_gate,
        dec_cache.reshape(seqs, span, wide),
        dec_gate,
        dec_lengths,
        w_out,
    )
    return pl.pallas_call(
        functools.partial(kernel, n, t),
        out_shape=(
            jax.ShapeDtypeStruct((count, outs), BF16),
            jax.ShapeDtypeStruct((seqs, outs), BF16),
        ),
        in_specs=[pl.BlockSpec(memory_space=pltpu.HBM)] * len(args),
        out_specs=(
            pl.BlockSpec(memory_space=pltpu.VMEM),
            pl.BlockSpec(memory_space=pltpu.VMEM),
        ),
        scratch_shapes=[
            pltpu.VMEM((count, width), BF16),
            pltpu.VMEM((seqs, width), BF16),
            pltpu.VMEM((1, width), F32),
            pltpu.VMEM((width, columns), BF16),
            pltpu.VMEM((wide, width), BF16),
            pltpu.VMEM((heads, width), BF16),
            pltpu.SMEM((heads,), F32),
            pltpu.VMEM((heads, count), F32),
            pltpu.VMEM((past + count, wide), BF16),
            pltpu.VMEM((past + count, wide), BF16),
            pltpu.VMEM((heads, past), F32),
            pltpu.VMEM((seqs, span, wide), BF16),
            pltpu.VMEM((seqs, heads, span), F32),
            pltpu.SMEM((seqs,), jnp.int32),
            pltpu.VMEM(w_out.shape, BF16),
            pltpu.VMEM((count + spare, width), BF16),
            pltpu.VMEM((seqs * heads, wide), F32),
            pltpu.VMEM((spare, columns), F32),
            pltpu.VMEM((n, count, columns), BF16),
            pltpu.VMEM((n, heads, wide), F32),
            pltpu.VMEM((n, count, columns), BF16),
            pltpu.VMEM((n, count, columns), BF16),
            pltpu.VMEM((n, heads, count), F32),
            pltpu.VMEM((n, heads, count), F32),
            pltpu.VMEM((t, count, columns), BF16),
            pltpu.VMEM((t, spare, columns), BF16),
            pltpu.VMEM((heads, count), F32),
            dma((len(args),)),
        ]
        + [dma((n,))] * 8
        + [dma((t,))] * 4,
        compiler_params=pltpu.CompilerParams(collective_id=0, has_side_effects=True),
    )(*args)


def solution(mesh):
    return jax.shard_map(
        functools.partial(local, mesh.shape["kv"], mesh.shape["tp"]),
        mesh=mesh,
        in_specs=(
            P(("grp", "kv"), None),
            P(("grp", "kv"), None),
            P(),
            P(None, "tp"),
            P(None, "tp"),
            P(None, "tp"),
            P(None, "tp"),
            P("tp"),
            P("tp", ("grp", "kv")),
            P(("grp", "kv"), "tp", None),
            P("tp", ("grp", "kv")),
            P(("grp", "kv"), None, "tp", None),
            P(("grp", "kv"), "tp", None),
            P(("grp", "kv")),
            P(None, "tp"),
        ),
        out_specs=(P(("grp", "kv"), "tp"), P(("grp", "kv"), "tp")),
        check_vma=False,
    )
```

```python
import functools
import math

import jax
import jax.numpy as jnp
from jax import lax
from jax.experimental import pallas as pl
from jax.experimental.pallas import tpu as pltpu
from jax.sharding import PartitionSpec as P

MESH = pl.DeviceIdType.MESH
LOG2E = math.log2(math.e)
F32 = jnp.float32
BF16 = jnp.bfloat16
HIGH = lax.Precision.HIGHEST


def dot_nt(a, b, precision=None):
    return lax.dot_general(
        a, b, (((1,), (1,)), ((), ())), preferred_element_type=F32, precision=precision
    )


def dot_nn(a, b, precision=None):
    return lax.dot_general(
        a, b, (((1,), (0,)), ((), ())), preferred_element_type=F32, precision=precision
    )


def dot_tn(a, b, precision=None):
    return lax.dot_general(
        a, b, (((0,), (0,)), ((), ())), preferred_element_type=F32, precision=precision
    )


def iota(shape, dim):
    return lax.broadcasted_iota(jnp.int32, shape, dim)


def loop(count, body, carry):
    if count <= 4:
        for k in range(count):
            carry = body(k, carry)
        return carry
    return lax.fori_loop(0, count, body, carry)


def normed_rows(rows, gain):
    wide = rows.astype(F32)
    scale = lax.rsqrt(jnp.mean(wide * wide, axis=-1, keepdims=True) + 1e-06)
    return wide * scale * gain


def kernel(
    n,
    t,
    piece_rows,
    dec_rows,
    gain_in,
    wq_in,
    wk_in,
    wv_in,
    wf_in,
    fb_in,
    decay_in,
    cache_in,
    cgate_in,
    dcache_in,
    dgate_in,
    lens_in,
    wo_in,
    piece_out,
    dec_out,
    rows,
    drows,
    gain,
    wq,
    wkv,
    wf,
    fb,
    decay,
    kv,
    vk,
    cgate,
    dcache,
    dgate,
    lens,
    wo,
    normed,
    qd,
    da,
    qbuf,
    tot,
    part,
    back,
    lse_part,
    lse_back,
    axp,
    axd,
    pbias,
    local_sem,
    q_send,
    q_recv,
    t_send,
    t_recv,
    p_send,
    p_recv,
    l_send,
    l_recv,
    a_send,
    a_recv,
    d_send,
    d_recv,
):
    me = lax.axis_index("kv")
    me_t = lax.axis_index("tp")
    count = piece_rows.shape[0]
    seqs = dec_rows.shape[0]
    past = cache_in.shape[0]
    wide = cache_in.shape[1]
    half = wide // 2
    heads = wf_in.shape[0]
    scale = half ** (-0.5) * LOG2E
    columns = heads * half

    def peer_at(k):
        down = n - 1 - k
        down = jnp.where(down <= me, down - 1, down)
        up = jnp.where(k >= me, k + 1, k)
        return jnp.where(me < n // 2, down, up)

    barrier = pltpu.get_barrier_semaphore()

    def greet(d, _):
        pl.semaphore_signal(
            barrier, inc=1, device_id={"kv": lax.rem(me + d + 1, n)}, device_id_type=MESH
        )
        return 0

    def greet_t(d, _):
        pl.semaphore_signal(
            barrier, inc=1, device_id={"tp": lax.rem(me_t + d + 1, t)}, device_id_type=MESH
        )
        return 0

    loop(n - 1, greet, 0)
    loop(t - 1, greet_t, 0)

    copies = {}
    for k, (name, src, dst) in enumerate(
        (
            ("rows", piece_rows, rows),
            ("drows", dec_rows, drows),
            ("gain", gain_in, gain),
            ("wq", wq_in, wq),
            ("wk", wk_in, wkv.at[pl.ds(0, half)]),
            ("wv", wv_in, wkv.at[pl.ds(half, half)]),
            ("wf", wf_in, wf),
            ("fb", fb_in, fb),
            ("decay", decay_in, decay),
            ("lens", lens_in, lens),
            ("dcache", dcache_in, dcache),
            ("dgate", dgate_in, dgate),
            ("cache", cache_in, kv.at[pl.ds(0, past)]),
            ("cgate", cgate_in, cgate),
            ("wo", wo_in, wo),
        )
    ):
        copy = pltpu.make_async_copy(src, dst, local_sem.at[k])
        copy.start()
        copies[name] = copy

    copies["rows"].wait()
    copies["drows"].wait()
    copies["gain"].wait()
    normed[0:count] = normed_rows(rows[...], gain[...]).astype(BF16)
    dec_normed = normed_rows(drows[...], gain[...])
    spare = normed.shape[0] - count
    normed[count:] = jnp.concatenate(
        [dec_normed, jnp.zeros((spare - seqs, dec_normed.shape[1]), F32)], axis=0
    ).astype(BF16)
    every = normed[...]
    copies["wf"].wait()
    copies["fb"].wait()
    copies["decay"].wait()
    raw = dot_nt(wf[...], every)
    row_of = iota((heads, 1), 0)
    bias = jnp.zeros((heads, 1), F32)
    for h in range(heads):
        bias = jnp.where(row_of == h, fb[h], bias)
    raw = raw + bias
    log_gate = jnp.minimum(raw, 0.0) - jnp.log1p(jnp.exp(-jnp.abs(raw)))
    piece_gate = log_gate[:, 0:count] + decay[...]
    upper = (iota((count, count), 0) <= iota((count, count), 1)).astype(F32)
    running = dot_nn(piece_gate, upper, HIGH)
    tot[0] = jnp.broadcast_to(running[:, count - 1 : count], tot.shape[1:])
    copies["wq"].wait()
    query = dot_nn(every, wq[...]).astype(BF16)
    qbuf[0] = query[0:count]

    pl.semaphore_wait(barrier, n - 1 + t - 1)

    def total_copy(peer):
        slot = lax.rem(peer - me + n, n)
        return pltpu.make_async_remote_copy(
            src_ref=tot.at[0],
            dst_ref=tot.at[slot],
            send_sem=t_send.at[slot],
            recv_sem=t_recv.at[slot],
            device_id={"kv": peer},
            device_id_type=MESH,
        )

    def query_copy(peer):
        slot = lax.rem(peer - me + n, n)
        return pltpu.make_async_remote_copy(
            src_ref=qbuf.at[0],
            dst_ref=qbuf.at[slot],
            send_sem=q_send.at[slot],
            recv_sem=q_recv.at[slot],
            device_id={"kv": peer},
            device_id_type=MESH,
        )

    def send_query(k, _):
        peer = peer_at(k)
        total_copy(peer).start()
        query_copy(peer).start()
        return 0

    loop(n - 1, send_query, 0)

    copies["wk"].wait()
    copies["wv"].wait()
    new_kv = dot_nt(every, wkv[...]).astype(BF16)
    copies["cache"].wait()
    kv[past : past + count] = new_kv[0:count]
    vk[...] = pltpu.roll(kv[...].astype(F32), half, 1).astype(BF16)
    copies["cgate"].wait()
    cgate[...] = cgate[...] * LOG2E

    lanes = seqs * heads
    qd[...] = jnp.zeros(qd.shape, F32)
    dec_query = query[count:].astype(F32)
    for b in range(seqs):
        for h in range(heads):
            qd[b * heads + h : b * heads + h + 1, 0:half] = dec_query[
                b : b + 1, h * half : (h + 1) * half
            ]
    q_dec = qd[...]
    dec_kv = new_kv[count:].astype(F32)
    copies["lens"].wait()
    copies["dgate"].wait()
    copies["dcache"].wait()
    span = dcache.shape[1]
    row = iota((lanes, 1), 0)
    length = jnp.zeros((lanes, 1), jnp.int32)
    own_kv = jnp.zeros((lanes, wide), F32)
    score = jnp.zeros((lanes, span), F32)
    for b in range(seqs):
        mine = (row >= b * heads) & (row < (b + 1) * heads)
        length = jnp.where(mine, lens[b], length)
        own_kv = jnp.where(mine, dec_kv[b : b + 1], own_kv)
        score = jnp.where(mine, dot_nt(q_dec.astype(BF16), dcache[b]), score)
    gate = jnp.concatenate([dgate[b] for b in range(seqs)], axis=0)
    new_gate = jnp.concatenate(
        [log_gate[:, count + b : count + b + 1] for b in range(seqs)], axis=0
    )
    place = iota((lanes, span), 1)
    last = jnp.sum(jnp.where(place == length - 1, gate, 0.0), axis=-1, keepdims=True)
    score = jnp.where(place < length, score * scale - gate * LOG2E, -jnp.inf)
    own = jnp.sum(q_dec * own_kv, axis=-1, keepdims=True) * scale - (last + new_gate) * LOG2E
    peak = jnp.maximum(jnp.max(score, axis=-1, keepdims=True), own)
    weight = jnp.exp2(score - peak)
    own_weight = jnp.exp2(own - peak)
    total = jnp.sum(weight, axis=-1, keepdims=True) + own_weight
    rounded = weight.astype(BF16)
    numer = own_weight.astype(BF16).astype(F32) * own_kv
    for b in range(seqs):
        mine = (row >= b * heads) & (row < (b + 1) * heads)
        numer = numer + jnp.where(mine, dot_nn(rounded, dcache[b]), 0.0)
    numer = numer / total
    da[...] = jnp.zeros(da.shape, F32)
    for b in range(seqs):
        for h in range(heads):
            at = b * heads + h
            da[b : b + 1, h * half : (h + 1) * half] = numer[at : at + 1, half:]
    axd[0] = da[...].astype(BF16)

    def head_copy(d, buf, send, recv):
        return pltpu.make_async_remote_copy(
            src_ref=buf.at[0],
            dst_ref=buf.at[d],
            send_sem=send.at[d],
            recv_sem=recv.at[d],
            device_id={"tp": lax.rem(me_t + d, t)},
            device_id_type=MESH,
        )

    for d in range(1, t):
        head_copy(d, axd, d_send, d_recv).start()

    def add_before(k, before):
        d = k + 1
        total_copy(lax.rem(me + d, n)).wait_recv()
        return before + jnp.where(d <= me, tot[d], 0.0)

    before = loop(n - 1, add_before, jnp.zeros(tot.shape[1:], F32))
    pbias[...] = -(running + before[:, 0:count]) * LOG2E

    low_lane = iota((count, wide), 1) < half
    low = jnp.where(low_lane, 1.0, 0.0).astype(BF16)
    high = jnp.where(low_lane, 0.0, 1.0).astype(BF16)
    lane = iota((count, wide), 1)

    def attend(q, seen):
        pairs = [q[:, p * wide : (p + 1) * wide] for p in range(heads // 2)]
        found = []
        stats = jnp.zeros((count, wide), F32)
        for odd, (mask, keys, values) in enumerate(((low, kv, vk), (high, vk, kv))):
            stacked = jnp.concatenate([p * mask for p in pairs], axis=0)
            old = dot_nt(stacked, keys[0:past])
            new = dot_nt(stacked, keys[past : past + count])
            old_weights, new_weights, sums = [], [], []
            for p in range(heads // 2):
                h = 2 * p + odd
                block = slice(p * count, (p + 1) * count)
                s_old = old[block] * scale + cgate[h : h + 1, :]
                s_new = jnp.where(seen, new[block] * scale + pbias[h : h + 1, :], -jnp.inf)
                top = jnp.maximum(
                    jnp.max(s_old, axis=-1, keepdims=True), jnp.max(s_new, axis=-1, keepdims=True)
                )
                w_old = jnp.exp2(s_old - top)
                w_new = jnp.exp2(s_new - top)
                amount = jnp.sum(w_old, axis=-1, keepdims=True) + jnp.sum(
                    w_new, axis=-1, keepdims=True
                )
                stats = jnp.where(lane == h, top + jnp.log2(amount), stats)
                old_weights.append(w_old.astype(BF16))
                new_weights.append(w_new.astype(BF16))
                sums.append(amount)
            out = dot_nn(jnp.concatenate(old_weights, axis=0), values[0:past])
            out = out + dot_nn(
                jnp.concatenate(new_weights, axis=0), values[past : past + count]
            )
            found.append(
                [out[p * count : (p + 1) * count] / sums[p] for p in range(heads // 2)]
            )
        merged = jnp.concatenate(
            [jnp.where(low_lane, found[0][p], found[1][p]) for p in range(heads // 2)], axis=1
        )
        return merged, jnp.transpose(stats)[0:heads, :]

    def part_copy(peer):
        slot = lax.rem(peer - me + n, n)
        return pltpu.make_async_remote_copy(
            src_ref=part.at[slot],
            dst_ref=back.at[slot],
            send_sem=p_send.at[slot],
            recv_sem=p_recv.at[slot],
            device_id={"kv": peer},
            device_id_type=MESH,
        )

    def lse_copy(peer):
        slot = lax.rem(peer - me + n, n)
        return pltpu.make_async_remote_copy(
            src_ref=lse_part.at[slot],
            dst_ref=lse_back.at[slot],
            send_sem=l_send.at[slot],
            recv_sem=l_recv.at[slot],
            device_id={"kv": peer},
            device_id_type=MESH,
        )

    def serve(k, _):
        peer = peer_at(n - 2 - k)
        came = lax.rem(me - peer + n, n)
        slot = lax.rem(peer - me + n, n)
        query_copy(lax.rem(me + came, n)).wait_recv()
        visible = iota((count, count), 0) * 0 + peer > me
        merged, lse = attend(qbuf[came], visible)
        part[slot] = merged.astype(BF16)
        lse_part[slot] = lse
        part_copy(peer).start()
        lse_copy(peer).start()
        return 0

    loop(n - 1, serve, 0)

    own_part, own_lse = attend(
        qbuf[0], iota((count, count), 1) <= iota((count, count), 0)
    )

    copies["wo"].wait()
    dec_mixed = jnp.zeros((axd.shape[1], wo.shape[1]), F32)
    for d in range(t):
        if d:
            head_copy(d, axd, d_send, d_recv).wait_recv()
        src = lax.rem(me_t - d + t, t)
        depth = pl.ds(pl.multiple_of(src * columns, columns), columns)
        dec_mixed = dec_mixed + dot_nn(axd[d], wo[depth, :])
    dec_out[...] = dec_mixed[0:seqs].astype(BF16)

    def top_of(k, top):
        d = k + 1
        lse_copy(lax.rem(me + d, n)).wait_recv()
        return jnp.maximum(top, lse_back[d])

    top = loop(n - 1, top_of, own_lse)
    own_share = jnp.exp2(own_lse - top)

    def sum_of(k, amount):
        return amount + jnp.exp2(lse_back[k + 1] - top)

    amount = loop(n - 1, sum_of, own_share)
    spread = (
        iota((heads, columns), 1) // half == iota((heads, columns), 0)
    ).astype(F32)

    def add_part(k, acc):
        d = k + 1
        share = dot_tn(jnp.exp2(lse_back[d] - top) / amount, spread, HIGH)
        part_copy(lax.rem(me + d, n)).wait_recv()
        return acc + back[d].astype(F32) * share

    attn = loop(n - 1, add_part, own_part * dot_tn(own_share / amount, spread, HIGH))
    axp[0] = attn.astype(BF16)
    for d in range(1, t):
        head_copy(d, axp, a_send, a_recv).start()
    mixed = jnp.zeros((count, wo.shape[1]), F32)
    for d in range(t):
        if d:
            head_copy(d, axp, a_send, a_recv).wait_recv()
        src = lax.rem(me_t - d + t, t)
        depth = pl.ds(pl.multiple_of(src * columns, columns), columns)
        mixed = mixed + dot_nn(axp[d], wo[depth, :])
    piece_out[...] = mixed.astype(BF16)

    def finish(k, _):
        peer = lax.rem(me + k + 1, n)
        total_copy(peer).wait_send()
        query_copy(peer).wait_send()
        part_copy(peer).wait_send()
        lse_copy(peer).wait_send()
        return 0

    loop(n - 1, finish, 0)
    for d in range(1, t):
        head_copy(d, axd, d_send, d_recv).wait_send()
        head_copy(d, axp, a_send, a_recv).wait_send()


def write_out(piece_in, dec_in, piece_out, dec_out, sem):
    first = pltpu.make_async_copy(piece_in, piece_out, sem.at[0])
    second = pltpu.make_async_copy(dec_in, dec_out, sem.at[1])
    first.start()
    second.start()
    first.wait()
    second.wait()


def local(
    n,
    t,
    piece_rows,
    dec_rows,
    norm_gain,
    w_query,
    w_key,
    w_value,
    w_forget,
    forget_bias,
    piece_decay,
    cache_kv,
    cache_gate,
    dec_cache,
    dec_gate,
    dec_lengths,
    w_out,
):
    count, width = piece_rows.shape
    seqs = dec_rows.shape[0]
    past, _, wide = cache_kv.shape
    half = wide // 2
    heads = w_forget.shape[1]
    columns = heads * half
    span = dec_cache.shape[1]
    outs = w_out.shape[1]
    spare = 16
    dma = pltpu.SemaphoreType.DMA
    args = (
        piece_rows,
        dec_rows,
        norm_gain.reshape(1, width),
        w_query,
        w_key.T,
        w_value.T,
        w_forget.T,
        forget_bias,
        piece_decay,
        cache_kv.reshape(past, wide),
        cache_gate,
        dec_cache.reshape(seqs, span, wide),
        dec_gate,
        dec_lengths,
        w_out,
    )
    args = tuple(pltpu.with_memory_space_constraint(a, pltpu.HBM) for a in args)
    mixed = pl.pallas_call(
        functools.partial(kernel, n, t),
        out_shape=(
            jax.ShapeDtypeStruct((count, outs), BF16),
            jax.ShapeDtypeStruct((seqs, outs), BF16),
        ),
        in_specs=[pl.BlockSpec(memory_space=pltpu.HBM)] * len(args),
        out_specs=(
            pl.BlockSpec(memory_space=pltpu.VMEM),
            pl.BlockSpec(memory_space=pltpu.VMEM),
        ),
        scratch_shapes=[
            pltpu.VMEM((count, width), BF16),
            pltpu.VMEM((seqs, width), BF16),
            pltpu.VMEM((1, width), F32),
            pltpu.VMEM((width, columns), BF16),
            pltpu.VMEM((wide, width), BF16),
            pltpu.VMEM((heads, width), BF16),
            pltpu.SMEM((heads,), F32),
            pltpu.VMEM((heads, count), F32),
            pltpu.VMEM((past + count, wide), BF16),
            pltpu.VMEM((past + count, wide), BF16),
            pltpu.VMEM((heads, past), F32),
            pltpu.VMEM((seqs, span, wide), BF16),
            pltpu.VMEM((seqs, heads, span), F32),
            pltpu.SMEM((seqs,), jnp.int32),
            pltpu.VMEM(w_out.shape, BF16),
            pltpu.VMEM((count + spare, width), BF16),
            pltpu.VMEM((seqs * heads, wide), F32),
            pltpu.VMEM((spare, columns), F32),
            pltpu.VMEM((n, count, columns), BF16),
            pltpu.VMEM((n, heads, wide), F32),
            pltpu.VMEM((n, count, columns), BF16),
            pltpu.VMEM((n, count, columns), BF16),
            pltpu.VMEM((n, heads, count), F32),
            pltpu.VMEM((n, heads, count), F32),
            pltpu.VMEM((t, count, columns), BF16),
            pltpu.VMEM((t, spare, columns), BF16),
            pltpu.VMEM((heads, count), F32),
            dma((len(args),)),
        ]
        + [dma((n,))] * 8
        + [dma((t,))] * 4,
        compiler_params=pltpu.CompilerParams(
            collective_id=0, has_side_effects=True, vmem_limit_bytes=24 * 1024 * 1024
        ),
    )(*args)
    return pl.pallas_call(
        write_out,
        out_shape=tuple(jax.ShapeDtypeStruct(m.shape, m.dtype) for m in mixed),
        in_specs=[pl.BlockSpec(memory_space=pltpu.VMEM)] * 2,
        out_specs=(pl.BlockSpec(memory_space=pltpu.HBM),) * 2,
        scratch_shapes=[dma((2,))],
        compiler_params=pltpu.CompilerParams(vmem_limit_bytes=4 * 1024 * 1024),
    )(*mixed)


def solution(mesh):
    return jax.shard_map(
        functools.partial(local, mesh.shape["kv"], mesh.shape["tp"]),
        mesh=mesh,
        in_specs=(
            P(("grp", "kv"), None),
            P(("grp", "kv"), None),
            P(),
            P(None, "tp"),
            P(None, "tp"),
            P(None, "tp"),
            P(None, "tp"),
            P("tp"),
            P("tp", ("grp", "kv")),
            P(("grp", "kv"), "tp", None),
            P("tp", ("grp", "kv")),
            P(("grp", "kv"), None, "tp", None),
            P(("grp", "kv"), "tp", None),
            P(("grp", "kv")),
            P(None, "tp"),
        ),
        out_specs=(P(("grp", "kv"), "tp"), P(("grp", "kv"), "tp")),
        check_vma=False,
    )
```

```python
import functools
import math

import jax
import jax.numpy as jnp
from jax import lax
from jax.experimental import pallas as pl
from jax.experimental.pallas import tpu as pltpu
from jax.sharding import PartitionSpec as P

MESH = pl.DeviceIdType.MESH
LOG2E = math.log2(math.e)
F32 = jnp.float32
BF16 = jnp.bfloat16
HIGH = lax.Precision.HIGHEST


def dot_nt(a, b, precision=None):
    return lax.dot_general(
        a, b, (((1,), (1,)), ((), ())), preferred_element_type=F32, precision=precision
    )


def dot_nn(a, b, precision=None):
    return lax.dot_general(
        a, b, (((1,), (0,)), ((), ())), preferred_element_type=F32, precision=precision
    )


def dot_tn(a, b, precision=None):
    return lax.dot_general(
        a, b, (((0,), (0,)), ((), ())), preferred_element_type=F32, precision=precision
    )


def iota(shape, dim):
    return lax.broadcasted_iota(jnp.int32, shape, dim)


def loop(count, body, carry):
    if count <= 4:
        for k in range(count):
            carry = body(k, carry)
        return carry
    return lax.fori_loop(0, count, body, carry)


def normed_rows(rows, gain):
    wide = rows.astype(F32)
    scale = lax.rsqrt(jnp.mean(wide * wide, axis=-1, keepdims=True) + 1e-06)
    return wide * scale * gain


def kernel(
    n,
    t,
    piece_rows,
    dec_rows,
    gain_in,
    wq_in,
    wk_in,
    wv_in,
    wf_in,
    fb_in,
    decay_in,
    cache_in,
    cgate_in,
    dcache_in,
    dgate_in,
    lens_in,
    wo_in,
    piece_out,
    dec_out,
    rows,
    drows,
    gain,
    wq,
    wkv,
    wf,
    fb,
    decay,
    kv,
    vk,
    cgate,
    dcache,
    dgate,
    lens,
    wo,
    normed,
    qd,
    da,
    qbuf,
    tot,
    part,
    back,
    lse_part,
    lse_back,
    axp,
    axd,
    pbias,
    local_sem,
    q_send,
    q_recv,
    t_send,
    t_recv,
    p_send,
    p_recv,
    l_send,
    l_recv,
    a_send,
    a_recv,
    d_send,
    d_recv,
):
    me = lax.axis_index("kv")
    me_t = lax.axis_index("tp")
    count = piece_rows.shape[0]
    seqs = dec_rows.shape[0]
    past = cache_in.shape[0]
    wide = cache_in.shape[1]
    half = wide // 2
    heads = wf_in.shape[0]
    scale = half ** (-0.5) * LOG2E
    columns = heads * half

    def peer_at(k):
        down = n - 1 - k
        down = jnp.where(down <= me, down - 1, down)
        up = jnp.where(k >= me, k + 1, k)
        return jnp.where(me < n // 2, down, up)

    barrier = pltpu.get_barrier_semaphore()

    def greet(d, _):
        pl.semaphore_signal(
            barrier, inc=1, device_id={"kv": lax.rem(me + d + 1, n)}, device_id_type=MESH
        )
        return 0

    def greet_t(d, _):
        pl.semaphore_signal(
            barrier, inc=1, device_id={"tp": lax.rem(me_t + d + 1, t)}, device_id_type=MESH
        )
        return 0

    loop(n - 1, greet, 0)
    loop(t - 1, greet_t, 0)

    copies = {}
    for k, (name, src, dst) in enumerate(
        (
            ("rows", piece_rows, rows),
            ("drows", dec_rows, drows),
            ("gain", gain_in, gain),
            ("wq", wq_in, wq),
            ("wk", wk_in, wkv.at[pl.ds(0, half)]),
            ("wv", wv_in, wkv.at[pl.ds(half, half)]),
            ("wf", wf_in, wf),
            ("fb", fb_in, fb),
            ("decay", decay_in, decay),
            ("lens", lens_in, lens),
            ("dcache", dcache_in, dcache),
            ("dgate", dgate_in, dgate),
            ("cache", cache_in, kv.at[pl.ds(0, past)]),
            ("cgate", cgate_in, cgate),
            ("wo", wo_in, wo),
        )
    ):
        copy = pltpu.make_async_copy(src, dst, local_sem.at[k])
        copies[name] = copy
    late = ("dcache", "dgate", "cache", "cgate", "wo")
    for name, copy in copies.items():
        if name not in late:
            copy.start()

    copies["rows"].wait()
    copies["drows"].wait()
    copies["gain"].wait()
    for name in late:
        copies[name].start()
    normed[0:count] = normed_rows(rows[...], gain[...]).astype(BF16)
    dec_normed = normed_rows(drows[...], gain[...])
    spare = normed.shape[0] - count
    normed[count:] = jnp.concatenate(
        [dec_normed, jnp.zeros((spare - seqs, dec_normed.shape[1]), F32)], axis=0
    ).astype(BF16)
    every = normed[...]
    copies["wf"].wait()
    copies["fb"].wait()
    copies["wq"].wait()
    copies["decay"].wait()
    query = dot_nn(every, wq[...]).astype(BF16)
    qbuf[0] = query[0:count]
    raw = dot_nt(wf[...], every)
    row_of = iota((heads, 1), 0)
    bias = jnp.zeros((heads, 1), F32)
    for h in range(heads):
        bias = jnp.where(row_of == h, fb[h], bias)
    raw = raw + bias
    log_gate = jnp.minimum(raw, 0.0) - jnp.log1p(jnp.exp(-jnp.abs(raw)))
    piece_gate = log_gate[:, 0:count] + decay[...]
    upper = (iota((count, count), 0) <= iota((count, count), 1)).astype(F32)
    running = dot_nn(piece_gate, upper, HIGH)
    tot[0] = jnp.broadcast_to(running[:, count - 1 : count], tot.shape[1:])

    pl.semaphore_wait(barrier, n - 1 + t - 1)

    def total_copy(peer):
        slot = lax.rem(peer - me + n, n)
        return pltpu.make_async_remote_copy(
            src_ref=tot.at[0],
            dst_ref=tot.at[slot],
            send_sem=t_send.at[slot],
            recv_sem=t_recv.at[slot],
            device_id={"kv": peer},
            device_id_type=MESH,
        )

    def query_copy(peer):
        slot = lax.rem(peer - me + n, n)
        return pltpu.make_async_remote_copy(
            src_ref=qbuf.at[0],
            dst_ref=qbuf.at[slot],
            send_sem=q_send.at[slot],
            recv_sem=q_recv.at[slot],
            device_id={"kv": peer},
            device_id_type=MESH,
        )

    def send_query(k, _):
        peer = peer_at(k)
        total_copy(peer).start()
        query_copy(peer).start()
        return 0

    loop(n - 1, send_query, 0)

    copies["wk"].wait()
    copies["wv"].wait()
    new_kv = dot_nt(every, wkv[...]).astype(BF16)
    copies["cache"].wait()
    kv[past : past + count] = new_kv[0:count]
    vk[...] = pltpu.roll(kv[...].astype(F32), half, 1).astype(BF16)
    copies["cgate"].wait()
    cgate[...] = cgate[...] * LOG2E

    lanes = seqs * heads
    qd[...] = jnp.zeros(qd.shape, F32)
    dec_query = query[count:].astype(F32)
    for b in range(seqs):
        for h in range(heads):
            qd[b * heads + h : b * heads + h + 1, 0:half] = dec_query[
                b : b + 1, h * half : (h + 1) * half
            ]
    q_dec = qd[...]
    dec_kv = new_kv[count:].astype(F32)
    copies["lens"].wait()
    copies["dgate"].wait()
    copies["dcache"].wait()
    span = dcache.shape[1]
    row = iota((lanes, 1), 0)
    length = jnp.zeros((lanes, 1), jnp.int32)
    own_kv = jnp.zeros((lanes, wide), F32)
    score = jnp.zeros((lanes, span), F32)
    for b in range(seqs):
        mine = (row >= b * heads) & (row < (b + 1) * heads)
        length = jnp.where(mine, lens[b], length)
        own_kv = jnp.where(mine, dec_kv[b : b + 1], own_kv)
        score = jnp.where(mine, dot_nt(q_dec.astype(BF16), dcache[b]), score)
    gate = jnp.concatenate([dgate[b] for b in range(seqs)], axis=0)
    new_gate = jnp.concatenate(
        [log_gate[:, count + b : count + b + 1] for b in range(seqs)], axis=0
    )
    place = iota((lanes, span), 1)
    last = jnp.sum(jnp.where(place == length - 1, gate, 0.0), axis=-1, keepdims=True)
    score = jnp.where(place < length, score * scale - gate * LOG2E, -jnp.inf)
    own = jnp.sum(q_dec * own_kv, axis=-1, keepdims=True) * scale - (last + new_gate) * LOG2E
    peak = jnp.maximum(jnp.max(score, axis=-1, keepdims=True), own)
    weight = jnp.exp2(score - peak)
    own_weight = jnp.exp2(own - peak)
    total = jnp.sum(weight, axis=-1, keepdims=True) + own_weight
    rounded = weight.astype(BF16)
    numer = own_weight.astype(BF16).astype(F32) * own_kv
    for b in range(seqs):
        mine = (row >= b * heads) & (row < (b + 1) * heads)
        numer = numer + jnp.where(mine, dot_nn(rounded, dcache[b]), 0.0)
    numer = numer / total
    da[...] = jnp.zeros(da.shape, F32)
    for b in range(seqs):
        for h in range(heads):
            at = b * heads + h
            da[b : b + 1, h * half : (h + 1) * half] = numer[at : at + 1, half:]
    axd[0] = da[...].astype(BF16)

    def head_copy(d, buf, send, recv):
        return pltpu.make_async_remote_copy(
            src_ref=buf.at[0],
            dst_ref=buf.at[d],
            send_sem=send.at[d],
            recv_sem=recv.at[d],
            device_id={"tp": lax.rem(me_t + d, t)},
            device_id_type=MESH,
        )

    for d in range(1, t):
        head_copy(d, axd, d_send, d_recv).start()

    def add_before(k, before):
        d = k + 1
        total_copy(lax.rem(me + d, n)).wait_recv()
        return before + jnp.where(d <= me, tot[d], 0.0)

    before = loop(n - 1, add_before, jnp.zeros(tot.shape[1:], F32))
    pbias[...] = -(running + before[:, 0:count]) * LOG2E

    low_lane = iota((count, wide), 1) < half
    low = jnp.where(low_lane, 1.0, 0.0).astype(BF16)
    high = jnp.where(low_lane, 0.0, 1.0).astype(BF16)
    lane = iota((count, wide), 1)

    def attend(q, seen):
        pairs = [q[:, p * wide : (p + 1) * wide] for p in range(heads // 2)]
        found = []
        stats = jnp.zeros((count, wide), F32)
        for odd, (mask, keys, values) in enumerate(((low, kv, vk), (high, vk, kv))):
            stacked = jnp.concatenate([p * mask for p in pairs], axis=0)
            old = dot_nt(stacked, keys[0:past])
            new = dot_nt(stacked, keys[past : past + count])
            old_weights, new_weights, sums = [], [], []
            for p in range(heads // 2):
                h = 2 * p + odd
                block = slice(p * count, (p + 1) * count)
                s_old = old[block] * scale + cgate[h : h + 1, :]
                s_new = jnp.where(seen, new[block] * scale + pbias[h : h + 1, :], -jnp.inf)
                top = jnp.maximum(
                    jnp.max(s_old, axis=-1, keepdims=True), jnp.max(s_new, axis=-1, keepdims=True)
                )
                w_old = jnp.exp2(s_old - top)
                w_new = jnp.exp2(s_new - top)
                amount = jnp.sum(w_old, axis=-1, keepdims=True) + jnp.sum(
                    w_new, axis=-1, keepdims=True
                )
                stats = jnp.where(lane == h, top + jnp.log2(amount), stats)
                old_weights.append(w_old.astype(BF16))
                new_weights.append(w_new.astype(BF16))
                sums.append(amount)
            out = dot_nn(jnp.concatenate(old_weights, axis=0), values[0:past])
            out = out + dot_nn(
                jnp.concatenate(new_weights, axis=0), values[past : past + count]
            )
            found.append(
                [out[p * count : (p + 1) * count] / sums[p] for p in range(heads // 2)]
            )
        merged = jnp.concatenate(
            [jnp.where(low_lane, found[0][p], found[1][p]) for p in range(heads // 2)], axis=1
        )
        return merged, jnp.transpose(stats)[0:heads, :]

    def part_copy(peer):
        slot = lax.rem(peer - me + n, n)
        return pltpu.make_async_remote_copy(
            src_ref=part.at[slot],
            dst_ref=back.at[slot],
            send_sem=p_send.at[slot],
            recv_sem=p_recv.at[slot],
            device_id={"kv": peer},
            device_id_type=MESH,
        )

    def lse_copy(peer):
        slot = lax.rem(peer - me + n, n)
        return pltpu.make_async_remote_copy(
            src_ref=lse_part.at[slot],
            dst_ref=lse_back.at[slot],
            send_sem=l_send.at[slot],
            recv_sem=l_recv.at[slot],
            device_id={"kv": peer},
            device_id_type=MESH,
        )

    def serve(k, _):
        peer = peer_at(n - 2 - k)
        came = lax.rem(me - peer + n, n)
        slot = lax.rem(peer - me + n, n)
        query_copy(lax.rem(me + came, n)).wait_recv()
        visible = iota((count, count), 0) * 0 + peer > me
        merged, lse = attend(qbuf[came], visible)
        lse_part[slot] = lse
        lse_copy(peer).start()
        part[slot] = merged.astype(BF16)
        part_copy(peer).start()
        return 0

    loop(n - 1, serve, 0)

    own_part, own_lse = attend(
        qbuf[0], iota((count, count), 1) <= iota((count, count), 0)
    )

    copies["wo"].wait()
    dec_mixed = jnp.zeros((axd.shape[1], wo.shape[1]), F32)
    for d in range(t):
        if d:
            head_copy(d, axd, d_send, d_recv).wait_recv()
        src = lax.rem(me_t - d + t, t)
        depth = pl.ds(pl.multiple_of(src * columns, columns), columns)
        dec_mixed = dec_mixed + dot_nn(axd[d], wo[depth, :])
    dec_out[...] = dec_mixed[0:seqs].astype(BF16)

    def top_of(k, top):
        d = k + 1
        lse_copy(lax.rem(me + d, n)).wait_recv()
        return jnp.maximum(top, lse_back[d])

    top = loop(n - 1, top_of, own_lse)
    own_share = jnp.exp2(own_lse - top)

    def sum_of(k, amount):
        return amount + jnp.exp2(lse_back[k + 1] - top)

    amount = loop(n - 1, sum_of, own_share)
    spread = (
        iota((heads, columns), 1) // half == iota((heads, columns), 0)
    ).astype(F32)

    def add_part(k, acc):
        d = k + 1
        share = dot_tn(jnp.exp2(lse_back[d] - top) / amount, spread, HIGH)
        part_copy(lax.rem(me + d, n)).wait_recv()
        return acc + back[d].astype(F32) * share

    attn = loop(n - 1, add_part, own_part * dot_tn(own_share / amount, spread, HIGH))
    axp[0] = attn.astype(BF16)
    for d in range(1, t):
        head_copy(d, axp, a_send, a_recv).start()
    mixed = jnp.zeros((count, wo.shape[1]), F32)
    for d in range(t):
        if d:
            head_copy(d, axp, a_send, a_recv).wait_recv()
        src = lax.rem(me_t - d + t, t)
        depth = pl.ds(pl.multiple_of(src * columns, columns), columns)
        mixed = mixed + dot_nn(axp[d], wo[depth, :])
    piece_out[...] = mixed.astype(BF16)

    def finish(k, _):
        peer = lax.rem(me + k + 1, n)
        total_copy(peer).wait_send()
        query_copy(peer).wait_send()
        part_copy(peer).wait_send()
        lse_copy(peer).wait_send()
        return 0

    loop(n - 1, finish, 0)
    for d in range(1, t):
        head_copy(d, axd, d_send, d_recv).wait_send()
        head_copy(d, axp, a_send, a_recv).wait_send()


def write_out(piece_in, dec_in, piece_out, dec_out, sem):
    first = pltpu.make_async_copy(piece_in, piece_out, sem.at[0])
    second = pltpu.make_async_copy(dec_in, dec_out, sem.at[1])
    first.start()
    second.start()
    first.wait()
    second.wait()


def local(
    n,
    t,
    piece_rows,
    dec_rows,
    norm_gain,
    w_query,
    w_key,
    w_value,
    w_forget,
    forget_bias,
    piece_decay,
    cache_kv,
    cache_gate,
    dec_cache,
    dec_gate,
    dec_lengths,
    w_out,
):
    count, width = piece_rows.shape
    seqs = dec_rows.shape[0]
    past, _, wide = cache_kv.shape
    half = wide // 2
    heads = w_forget.shape[1]
    columns = heads * half
    span = dec_cache.shape[1]
    outs = w_out.shape[1]
    spare = 16
    dma = pltpu.SemaphoreType.DMA
    args = (
        piece_rows,
        dec_rows,
        norm_gain.reshape(1, width),
        w_query,
        w_key.T,
        w_value.T,
        w_forget.T,
        forget_bias,
        piece_decay,
        cache_kv.reshape(past, wide),
        cache_gate,
        dec_cache.reshape(seqs, span, wide),
        dec_gate,
        dec_lengths,
        w_out,
    )
    args = tuple(pltpu.with_memory_space_constraint(a, pltpu.HBM) for a in args)
    mixed = pl.pallas_call(
        functools.partial(kernel, n, t),
        out_shape=(
            jax.ShapeDtypeStruct((count, outs), BF16),
            jax.ShapeDtypeStruct((seqs, outs), BF16),
        ),
        in_specs=[pl.BlockSpec(memory_space=pltpu.HBM)] * len(args),
        out_specs=(
            pl.BlockSpec(memory_space=pltpu.VMEM),
            pl.BlockSpec(memory_space=pltpu.VMEM),
        ),
        scratch_shapes=[
            pltpu.VMEM((count, width), BF16),
            pltpu.VMEM((seqs, width), BF16),
            pltpu.VMEM((1, width), F32),
            pltpu.VMEM((width, columns), BF16),
            pltpu.VMEM((wide, width), BF16),
            pltpu.VMEM((heads, width), BF16),
            pltpu.SMEM((heads,), F32),
            pltpu.VMEM((heads, count), F32),
            pltpu.VMEM((past + count, wide), BF16),
            pltpu.VMEM((past + count, wide), BF16),
            pltpu.VMEM((heads, past), F32),
            pltpu.VMEM((seqs, span, wide), BF16),
            pltpu.VMEM((seqs, heads, span), F32),
            pltpu.SMEM((seqs,), jnp.int32),
            pltpu.VMEM(w_out.shape, BF16),
            pltpu.VMEM((count + spare, width), BF16),
            pltpu.VMEM((seqs * heads, wide), F32),
            pltpu.VMEM((spare, columns), F32),
            pltpu.VMEM((n, count, columns), BF16),
            pltpu.VMEM((n, heads, wide), F32),
            pltpu.VMEM((n, count, columns), BF16),
            pltpu.VMEM((n, count, columns), BF16),
            pltpu.VMEM((n, heads, count), F32),
            pltpu.VMEM((n, heads, count), F32),
            pltpu.VMEM((t, count, columns), BF16),
            pltpu.VMEM((t, spare, columns), BF16),
            pltpu.VMEM((heads, count), F32),
            dma((len(args),)),
        ]
        + [dma((n,))] * 8
        + [dma((t,))] * 4,
        compiler_params=pltpu.CompilerParams(
            collective_id=0, has_side_effects=True, vmem_limit_bytes=24 * 1024 * 1024
        ),
    )(*args)
    return pl.pallas_call(
        write_out,
        out_shape=tuple(jax.ShapeDtypeStruct(m.shape, m.dtype) for m in mixed),
        in_specs=[pl.BlockSpec(memory_space=pltpu.VMEM)] * 2,
        out_specs=(pl.BlockSpec(memory_space=pltpu.HBM),) * 2,
        scratch_shapes=[dma((2,))],
        compiler_params=pltpu.CompilerParams(vmem_limit_bytes=4 * 1024 * 1024),
    )(*mixed)


def solution(mesh):
    return jax.shard_map(
        functools.partial(local, mesh.shape["kv"], mesh.shape["tp"]),
        mesh=mesh,
        in_specs=(
            P(("grp", "kv"), None),
            P(("grp", "kv"), None),
            P(),
            P(None, "tp"),
            P(None, "tp"),
            P(None, "tp"),
            P(None, "tp"),
            P("tp"),
            P("tp", ("grp", "kv")),
            P(("grp", "kv"), "tp", None),
            P("tp", ("grp", "kv")),
            P(("grp", "kv"), None, "tp", None),
            P(("grp", "kv"), "tp", None),
            P(("grp", "kv")),
            P(None, "tp"),
        ),
        out_specs=(P(("grp", "kv"), "tp"), P(("grp", "kv"), "tp")),
        check_vma=False,
    )
```
